256 devices in a mesh: kv: 32 (over z, y), tp: 8 (over x, core).
Axes of the slice: x: 4, y: 4, z: 8, core: 2. Of those that a mesh axis runs over, the one named last changes fastest.
Arguments:
- tokens: bfloat16 [32, 4096], P(None, ('kv', 'tp')), may hold values from -24 to 24
- attention_norm_gain: float32 [4096], P('kv'), may hold values from 0.1 to 1.9
- query_first: bfloat16 [4096, 2048], P('kv', 'tp'), may hold values from -0.09375 to 0.09375
- query_second: bfloat16 [4096, 2048], P('kv', 'tp'), may hold values from -0.09375 to 0.09375
- key_first: bfloat16 [4096, 512], P('kv', 'tp'), may hold values from -0.15625 to 0.15625
- key_second: bfloat16 [4096, 512], P('kv', 'tp'), may hold values from -0.15625 to 0.15625
- value_weight: bfloat16 [4096, 1024], P('kv', 'tp'), may hold values from -0.09375 to 0.09375
- key_cache: bfloat16 [32, 16384, 8, 128], P(None, 'kv', 'tp'), may hold values from -270 to 270
- value_cache: bfloat16 [32, 16384, 8, 128], P(None, 'kv', 'tp'), may hold values from -6 to 6
- lambdas: float32 [32], P('tp'), may hold values from 0.3 to 0.8
- head_gain: float32 [128], replicated, may hold values from 0.1 to 1.9
- out_weight: bfloat16 [4096, 4096], P('tp', 'kv'), may hold values from -0.09375 to 0.09375
- mlp_gain: float32 [4096], P('kv'), may hold values from 0.1 to 1.9
- gate_weight: bfloat16 [4096, 11264], P('kv', 'tp'), may hold values from -0.09375 to 0.09375
- up_weight: bfloat16 [4096, 11264], P('kv', 'tp'), may hold values from -0.09375 to 0.09375
- down_projection_weight: bfloat16 [11264, 4096], P('tp', 'kv'), may hold values from -0.109375 to 0.109375
Outputs:
- layer_out: bfloat16 [32, 4096], P(None, ('kv', 'tp'))
- incoming_key_pair: bfloat16 [32, 8, 128], P(None, 'tp')
- new_values: bfloat16 [32, 8, 128], P(None, 'tp')
The draws below stay inside these ranges and needn't reach their ends.
All inputs are finite; a program needn't handle non-finite values.
Results may differ from the reference program's by a relative error of at most 0.014.
Values may be sent and summed in bfloat16 or wider, within the bound.
A program may use at most 64 MiB of HBM per device.

```python
import math
import jax
import jax.numpy as jnp
from jax import lax

D = 4096
HEADS = 32
KV_HEADS = 8
HEAD_DIM = 64
FF = 11264
BATCH = 32
CONTEXT = 16384
N_TP = 8


def draw_tokens(key, part):
    key_base = jax.random.fold_in(key, 11)
    key_rough = jax.random.fold_in(key, 12)
    rough = jax.random.uniform(key_rough, (D,), jnp.float32, 0.6, 1.4)
    base = jnp.clip(jax.random.normal(key_base, (BATCH, D), jnp.float32), -4.0, 4.0)
    ramp = jnp.exp(jnp.linspace(0.0, math.log(4.0), D)).astype(jnp.float32)
    return (base * ramp[None, :] * rough[None, :]).astype(jnp.bfloat16)


def draw_key_cache(key, part):
    key_base = jax.random.fold_in(key, 21)
    shape = (BATCH, CONTEXT, KV_HEADS, 2 * HEAD_DIM)
    base = 1.75 * jnp.clip(jax.random.normal(key_base, shape, jnp.float32), -4.0, 4.0)
    return base.astype(jnp.bfloat16)


def block_scale(own_key, shape, split, least, high):
    factor_of = 1.0
    for dim, parts in split:
        draws = jax.random.uniform(jax.random.fold_in(jax.random.fold_in(own_key, 6), dim), (parts,), jnp.float32, least / len(split), high / len(split))
        factor_of = factor_of * jnp.repeat(jnp.exp(draws), shape[dim] // parts).reshape((-1,) + (1,) * (len(shape) - 1 - dim))
    return factor_of


def noise(rng, shape, deviation, reach, shards=(), held_as=jnp.bfloat16):
    level = block_scale(rng, shape, shards, -0.22, 0.18) if shards else 1.0
    array = jax.random.normal(rng, shape, jnp.float32) * deviation * level
    return jnp.minimum(jnp.maximum(array, -reach), reach).astype(held_as)


def setup_inputs(seed: int = 0) -> dict:
    key_of = jax.random.split(jax.random.key(seed), 17)
    return {
        "tokens": draw_tokens(jax.random.fold_in(key_of[16], 71), 0),
        "attention_norm_gain": jnp.clip(1.0 + 0.18 * jax.random.normal(key_of[1], (D,), jnp.float32), 0.1, 1.9),
        "query_first": noise(key_of[2], (D, HEADS * HEAD_DIM), D ** -0.5, 0.09375, ((0, 32), (1, 8))),
        "query_second": noise(key_of[3], (D, HEADS * HEAD_DIM), D ** -0.5, 0.09375, ((0, 32), (1, 8))),
        "key_first": noise(key_of[4], (D, KV_HEADS * HEAD_DIM), (D // 3) ** -0.5, 0.15625, ((0, 32), (1, 8))),
        "key_second": noise(key_of[5], (D, KV_HEADS * HEAD_DIM), (D // 3) ** -0.5, 0.15625, ((0, 32), (1, 8))),
        "value_weight": noise(key_of[6], (D, KV_HEADS * 2 * HEAD_DIM), D ** -0.5, 0.09375, ((0, 32), (1, 8))),
        "key_cache": draw_key_cache(jax.random.fold_in(key_of[16], 71), 0),
        "value_cache": noise(key_of[8], (BATCH, CONTEXT, KV_HEADS, 2 * HEAD_DIM), 1.0, 6.0, ((1, 32), (2, 8))),
        "lambdas": jnp.clip(0.3 + 0.5 * jax.random.uniform(key_of[9], (HEADS,), jnp.float32) ** block_scale(key_of[9], (HEADS,), ((0, 8),), -0.2, 0.2), 0.3, 0.8),
        "head_gain": jnp.clip(1.0 + 0.18 * jax.random.normal(key_of[10], (2 * HEAD_DIM,), jnp.float32), 0.1, 1.9),
        "out_weight": noise(key_of[11], (HEADS * 2 * HEAD_DIM, D), (HEADS * 2 * HEAD_DIM) ** -0.5, 0.09375, ((0, 8), (1, 32))),
        "mlp_gain": jnp.clip(1.0 + 0.18 * jax.random.normal(key_of[12], (D,), jnp.float32), 0.1, 1.9),
        "gate_weight": noise(key_of[13], (D, FF), D ** -0.5, 0.09375, ((0, 32), (1, 8))),
        "up_weight": noise(key_of[14], (D, FF), D ** -0.5, 0.09375, ((0, 32), (1, 8))),
        "down_projection_weight": noise(key_of[15], (FF, D), (FF // 4) ** -0.5, 0.109375, ((0, 8), (1, 32))),
    }


EPS = 1e-06

def blocked_product(left, right, blocks):
    width = left.shape[1] // blocks
    total = jnp.zeros((left.shape[0], right.shape[1]), jnp.float32)
    for index in range(blocks):
        part = jnp.dot(left[:, index * width:(index + 1) * width], right[index * width:(index + 1) * width], preferred_element_type=jnp.float32)
        total = total + lax.optimization_barrier(part.astype(jnp.bfloat16)).astype(jnp.float32)
    return total.astype(jnp.bfloat16)

def reference(tokens, attention_norm_gain, query_first, query_second, key_first, key_second, value_weight, key_cache, value_cache, lambdas, head_gain, out_weight, mlp_gain, gate_weight, up_weight, down_projection_weight):
    batch = tokens.shape[0]
    group = HEADS // KV_HEADS
    wide = tokens.astype(jnp.float32)
    scaled = (wide * attention_norm_gain).astype(jnp.bfloat16)
    factor = lax.rsqrt(lax.optimization_barrier(jnp.mean(wide * wide, axis=1, keepdims=True)) + EPS)

    def project(weight):
        return (jnp.dot(scaled, weight, preferred_element_type=jnp.float32) * factor).astype(jnp.bfloat16)
    query_one = project(query_first).reshape(batch, HEADS, HEAD_DIM)
    query_two = project(query_second).reshape(batch, HEADS, HEAD_DIM)
    key_one = project(key_first).reshape(batch, KV_HEADS, HEAD_DIM)
    key_two = project(key_second).reshape(batch, KV_HEADS, HEAD_DIM)
    value_new = project(value_weight).reshape(batch, KV_HEADS, 2 * HEAD_DIM)
    incoming_key_pair = jnp.concatenate([key_one, key_two], axis=2)
    scale = HEAD_DIM ** (-0.5)

    def attend(items):
        query_a, query_b, cached_keys, cached_values, incoming_key, fresh_value = items
        all_keys = jnp.concatenate([cached_keys, incoming_key[None]], axis=0).astype(jnp.float32)
        all_values = jnp.concatenate([cached_values, fresh_value[None]], axis=0).astype(jnp.float32)
        results = []
        for which, current_query in enumerate((query_a, query_b)):
            grouped = current_query.reshape(KV_HEADS, group, HEAD_DIM).astype(jnp.float32)
            part = all_keys[:, :, which * HEAD_DIM:(which + 1) * HEAD_DIM]
            scores = jnp.einsum('kgd,pkd->kgp', grouped, part) * scale
            top = lax.optimization_barrier(jnp.max(scores, axis=2, keepdims=True))
            expo = jnp.exp(scores - top)
            total = lax.optimization_barrier(jnp.sum(expo, axis=2, keepdims=True))
            rounded = lax.optimization_barrier(expo.astype(jnp.bfloat16)).astype(jnp.float32)
            weighted = jnp.einsum('kgp,pkv->kgv', rounded, all_values)
            results.append((weighted / total).reshape(HEADS, 2 * HEAD_DIM))
        return (results[0], results[1])
    first_map, second_attention_map = lax.map(attend, (query_one, query_two, key_cache, value_cache, incoming_key_pair, value_new))
    mixed = first_map - lambdas[None, :, None] * second_attention_map
    normed = mixed * lax.rsqrt(lax.optimization_barrier(jnp.mean(mixed * mixed, axis=2, keepdims=True)) + EPS) * head_gain
    heads_out = normed.astype(jnp.bfloat16).reshape(batch, HEADS * 2 * HEAD_DIM)
    attn = blocked_product(heads_out, out_weight, N_TP)
    middle = (wide + attn.astype(jnp.float32)).astype(jnp.bfloat16)
    wide_mid = middle.astype(jnp.float32)
    scaled_mid = (wide_mid * mlp_gain).astype(jnp.bfloat16)
    factor_mid = lax.rsqrt(lax.optimization_barrier(jnp.mean(wide_mid * wide_mid, axis=1, keepdims=True)) + EPS)
    gate = jnp.dot(scaled_mid, gate_weight, preferred_element_type=jnp.float32) * factor_mid
    upward = jnp.dot(scaled_mid, up_weight, preferred_element_type=jnp.float32) * factor_mid
    hidden = (jax.nn.silu(gate) * upward).astype(jnp.bfloat16)
    feed = blocked_product(hidden, down_projection_weight, N_TP)
    layer_out = (wide_mid + feed.astype(jnp.float32)).astype(jnp.bfloat16)
    return (layer_out, incoming_key_pair, value_new)
```

```python
import functools

import jax
import jax.numpy as jnp
from jax import lax
from jax.experimental import pallas as pl
from jax.experimental.pallas import tpu as pltpu
from jax.sharding import PartitionSpec as P

D = 4096
HD = 64
EPS = 1e-06
NZ, NY = 8, 4
KV = NZ * NY
TP = 8
F32 = jnp.float32
BF16 = jnp.bfloat16
MESH = pl.DeviceIdType.MESH

Z_DIST = [min(k, NZ - k) for k in range(NZ)]
Y_DIST = [min(k, NY - k) for k in range(NY)]
OFFSETS = sorted(
    [(dz, dy) for dz in range(NZ) for dy in range(NY) if (dz, dy) != (0, 0)],
    key=lambda o: -(Z_DIST[o[0]] + Y_DIST[o[1]]),
)


def kernel(
    tok_h, an_gain_h, wq1_h, wq2_h, wk1_h, wk2_h, wv_h, k_h, v_h, lam_h, hg_h, wo_h, mg_h, wg_h,
    wu_h, wd_h,
    out_ref, kp_ref, nv_ref,
    an_gain, wq1, wq2, wq, wk, wv, keys, vals, lam, hg, wo, mg, wg, wu, wd,
    tok, b1_s, b1_r, b2_s, b2_r, c1_s, c1_r, c2_s, c2_r, c2_f, d_s, d_r, e1_f, e1_s, e1_r, e2_s,
    e2_r, e2_f, mid_t, f_s, f_r,
    ld, tok_ss, tok_rs, b1_ss, b1_rs, b2_ss, b2_rs, c1_ss, c1_rs, c2_ss, c2_rs, d_ss, d_rs,
    e1_ss, e1_rs, e2_ss, e2_rs, f_ss, f_rs,
):
    kv = lax.axis_index("kv")
    tp = lax.axis_index("tp")
    mz, my = kv // NY, kv % NY

    def kv_peer(dz, dy):
        return ((mz + dz) % NZ) * NY + (my + dy) % NY

    def tp_peer(k):
        return (tp + k) % TP

    loads = []

    def load(src, dst):
        copy = pltpu.make_async_copy(src, dst, ld.at[len(loads)])
        copy.start()
        loads.append(copy)
        return copy

    l_tok = load(tok_h, tok.at[tp])
    l_ag = load(an_gain_h, an_gain)
    l_w = [
        load(wq1_h, wq1), load(wq2_h, wq2), load(wk1_h, wk.at[pl.ds(0, HD)]),
        load(wk2_h, wk.at[pl.ds(HD, HD)]), load(wv_h, wv),
    ]

    barrier = pltpu.get_barrier_semaphore()
    for dz, dy in OFFSETS:
        pl.semaphore_signal(barrier, inc=1, device_id=(kv_peer(dz, dy), tp), device_id_type=MESH)
    for k in range(1, TP):
        pl.semaphore_signal(barrier, inc=1, device_id=(kv, tp_peer(k)), device_id_type=MESH)

    l_k = [load(k_h.at[pl.ds(8 * i, 8)], keys.at[pl.ds(8 * i, 8)]) for i in range(4)]
    l_v = [load(v_h.at[pl.ds(8 * i, 8)], vals.at[pl.ds(8 * i, 8)]) for i in range(4)]
    l_lam = load(lam_h, lam)
    l_hg = load(hg_h, hg)
    l_wo = load(wo_h, wo)
    l_mg = load(mg_h, mg)
    l_gu = [load(wg_h, wg), load(wu_h, wu)]
    l_wd = load(wd_h, wd)

    def send(src, dst, ss, rs, device):
        copy = pltpu.make_async_remote_copy(
            src_ref=src, dst_ref=dst, send_sem=ss, recv_sem=rs, device_id=device,
            device_id_type=MESH,
        )
        copy.start()

    def all_in(ref, sem):
        pltpu.make_async_copy(ref, ref, sem).wait()

    for c in l_w:
        c.wait()
    for h in range(4):
        wq[:, 128 * h : 128 * h + 128] = jnp.concatenate(
            [wq1[:, HD * h : HD * h + HD], wq2[:, HD * h : HD * h + HD]], axis=1
        )
    b1_s[...] = jnp.zeros_like(b1_s)
    e1_f[...] = jnp.zeros_like(e1_f)
    l_tok.wait()
    l_ag.wait()
    pl.semaphore_wait(barrier, KV - 1 + TP - 1)

    for k in (4, 5, 3, 2, 6, 7, 1):
        send(tok.at[tp], tok.at[tp], tok_ss, tok_rs, (kv, tp_peer(k)))
    all_in(tok.at[pl.ds(0, TP - 1)], tok_rs)
    x = tok[...].astype(F32).reshape(TP * 16, KV).T
    scaled = (x * an_gain[...]).astype(BF16)
    sq = jnp.sum(x * x, axis=1, keepdims=True)
    b1_s[pl.ds(6, KV, stride=8), :] = jnp.broadcast_to(sq, (KV, 128))
    pq = jnp.dot(scaled, wq[...], preferred_element_type=F32)
    for h in range(4):
        b1_s[pl.ds(h, KV, stride=8), :] = pq[:, 128 * h : 128 * h + 128]
    b1_s[pl.ds(4, KV, stride=8), :] = lax.dot_general(
        scaled, wk[...], (((1,), (1,)), ((), ())), preferred_element_type=F32
    )
    b1_s[pl.ds(5, KV, stride=8), :] = jnp.dot(scaled, wv[...], preferred_element_type=F32)

    def rows(ref, i, n):
        return ref.at[pl.ds(pl.multiple_of(i * n, n), n)]

    for dz, dy in OFFSETS:
        p = kv_peer(dz, dy)
        send(rows(b1_s, p, 8), rows(b1_r, kv, 8), b1_ss, b1_rs, (p, tp))
    own = pl.ds(pl.multiple_of(kv * 8, 8), 8)
    b1_r[own, :] = b1_s[own, :]
    all_in(b1_r.at[pl.ds(0, (KV - 1) * 8)], b1_rs)
    total = jnp.sum(b1_r[...].reshape(KV, 8, 128), axis=0)
    factor = lax.rsqrt(total[6:7] / D + EPS)
    proj = (total * factor).astype(BF16).astype(F32)
    lane = lax.broadcasted_iota(jnp.int32, (8, 128), 1)
    row = lax.broadcasted_iota(jnp.int32, (8, 128), 0)
    both = jnp.concatenate([proj[0:4], proj[0:4]], axis=0)
    query = jnp.where((lane < HD) == (row < 4), both, 0.0)
    b2_s[...] = query.astype(BF16)

    for dz, dy in OFFSETS:
        send(b2_s, b2_r.at[kv], b2_ss, b2_rs.at[kv], (kv_peer(dz, dy), tp))
    b2_r[kv] = query.astype(BF16)
    scale = HD ** (-0.5)
    new_key, new_value = proj[4:5], proj[5:6]
    fresh = jnp.sum(query * new_key, axis=1, keepdims=True) * scale

    for c in l_k + l_v:
        c.wait()

    def attend(g, carry):
        half = (g + 1) // 2
        dz = (g % 2) * half + (1 - g % 2) * ((NZ - half) % NZ)
        base = ((mz + dz) % NZ) * NY
        for j in range(NY):
            s = base + j

            @pl.when(s != kv)
            def _():
                pltpu.make_async_copy(b2_r.at[s], b2_r.at[s], b2_rs.at[s]).wait()

        lane16 = lax.broadcasted_iota(jnp.int32, (8, 128), 1)
        for j in range(NY):
            s = base + j
            score = (
                lax.dot_general(
                    b2_r[s], keys[s], (((1,), (1,)), ((), ())), preferred_element_type=F32
                )
                * scale
            )
            top = jnp.max(score, axis=1, keepdims=True)
            expo = jnp.exp(score - top)
            tot = jnp.sum(expo, axis=1, keepdims=True)
            value = jnp.dot(expo.astype(BF16), vals[s], preferred_element_type=F32) / tot
            level = jnp.broadcast_to(top + jnp.log(tot), (8, 128))
            p1 = level.astype(BF16).astype(F32)
            p2 = (level - p1).astype(BF16).astype(F32)
            p3 = level - p1 - p2
            pieces = jnp.where(
                lane16 == 0, p1, jnp.where(lane16 == 1, p2, jnp.where(lane16 == 2, p3, 0.0))
            )
            c1_s[s] = jnp.concatenate([value, pieces], axis=0).astype(BF16)
        for j in range(NY):
            s = base + j

            @pl.when(s != kv)
            def _():
                send(c1_s.at[s], c1_r.at[kv], c1_ss, c1_rs, (s, tp))

        return carry

    lax.fori_loop(0, NZ, attend, 0)
    c1_r[kv] = c1_s[kv]

    for c in (l_lam, l_hg, l_wo, l_mg):
        c.wait()
    r4 = lax.broadcasted_iota(jnp.int32, (4, 128), 0)
    lam_rows = jnp.where(
        r4 == 0, lam[0], jnp.where(r4 == 1, lam[1], jnp.where(r4 == 2, lam[2], lam[3]))
    )
    all_in(c1_r.at[pl.ds(0, KV - 1)], c1_rs)
    states = c1_r[...].astype(F32)
    values = states[:, 0:8, :]
    levels = jnp.sum(states[:, 8:16, :], axis=2, keepdims=True)
    top = jnp.maximum(jnp.max(levels, axis=0), fresh)
    weight = jnp.exp(levels - top[None])
    fresh_weight = jnp.exp(fresh - top)
    total_w = jnp.sum(weight, axis=0) + fresh_weight
    merged = (jnp.sum(values * weight, axis=0) + fresh_weight * new_value) / total_w
    mixed = merged[0:4] - lam_rows * merged[4:8]
    normed = (
        mixed * lax.rsqrt(jnp.mean(mixed * mixed, axis=1, keepdims=True) + EPS) * hg[...]
    )
    c2 = jnp.concatenate([normed, proj[4:6], jnp.zeros((2, 128), F32)], axis=0).astype(BF16)
    c2_s[...] = c2

    for dz, dy in OFFSETS:
        send(c2_s, c2_r.at[kv], c2_ss, c2_rs, (kv_peer(dz, dy), tp))
    c2_r[kv] = c2
    all_in(c2_r.at[pl.ds(0, KV - 1)], c2_rs)
    c2_f[...] = c2_r[...].astype(F32).reshape(KV * 8, 128)
    heads = jnp.concatenate(
        [c2_f[pl.ds(h, KV, stride=8), :].astype(BF16) for h in range(4)], axis=1
    )
    attn_part = jnp.dot(heads, wo[...], preferred_element_type=F32).astype(BF16)
    d_s[...] = attn_part

    for k in (4, 5, 3, 2, 6, 7, 1):
        send(d_s, d_r.at[tp], d_ss, d_rs, (kv, tp_peer(k)))
    d_r[tp] = attn_part
    kp_ref[...] = c2_f[pl.ds(4, KV, stride=8), :].astype(BF16)
    nv_ref[...] = c2_f[pl.ds(5, KV, stride=8), :].astype(BF16)
    all_in(d_r.at[pl.ds(0, TP - 1)], d_rs)
    attn = jnp.sum(d_r[...].astype(F32), axis=0).astype(BF16).astype(F32)
    middle = (x + attn).astype(BF16).astype(F32)
    scaled_mid = (middle * mg[...]).astype(BF16)
    sq_mid = jnp.broadcast_to(jnp.sum(middle * middle, axis=1, keepdims=True), (KV, 128))
    for c in l_gu:
        c.wait()
    lane32 = lax.broadcasted_iota(jnp.int32, (KV, 128), 1)
    s1 = sq_mid.astype(BF16).astype(F32)
    s2 = (sq_mid - s1).astype(BF16).astype(F32)
    e1_f[pl.ds(22, KV, stride=24), :] = jnp.where(
        lane32 == 0, s1, jnp.where(lane32 == 1, s2, jnp.where(lane32 == 2, sq_mid - s1 - s2, 0.0))
    )
    gate = jnp.dot(scaled_mid, wg[...], preferred_element_type=F32)
    for c in range(11):
        e1_f[pl.ds(c, KV, stride=24), :] = gate[:, 128 * c : 128 * c + 128]
    up = jnp.dot(scaled_mid, wu[...], preferred_element_type=F32)
    for c in range(11):
        e1_f[pl.ds(11 + c, KV, stride=24), :] = up[:, 128 * c : 128 * c + 128]
    e1_s[...] = e1_f[...].reshape(KV * 3, 8, 128).astype(BF16)

    def thirds(ref, i):
        return ref.at[pl.ds(i * 3, 3)]

    for dz, dy in OFFSETS:
        p = kv_peer(dz, dy)
        send(thirds(e1_s, p), thirds(e1_r, kv), e1_ss, e1_rs, (p, tp))
    e1_r[pl.ds(kv * 3, 3)] = e1_s[pl.ds(kv * 3, 3)]
    mid_t[...] = middle.T.reshape(TP, 16, KV)
    all_in(e1_r.at[pl.ds(0, (KV - 1) * 3)], e1_rs)
    sums = jnp.sum(e1_r[...].astype(F32).reshape(KV, 24, 128), axis=0)
    factor_mid = lax.rsqrt(jnp.sum(sums[22:23], axis=1, keepdims=True) / D + EPS)
    gate_all = sums[0:11] * factor_mid
    up_all = sums[11:22] * factor_mid
    hidden = gate_all / (1.0 + jnp.exp(-gate_all)) * up_all
    hidden = jnp.concatenate([hidden, jnp.zeros((5, 128), F32)], axis=0).astype(BF16)
    e2_s[...] = hidden

    for dz, dy in OFFSETS:
        send(e2_s, e2_r.at[kv], e2_ss, e2_rs, (kv_peer(dz, dy), tp))
    e2_r[kv] = hidden
    l_wd.wait()
    all_in(e2_r.at[pl.ds(0, KV - 1)], e2_rs)
    e2_f[...] = e2_r[...].astype(F32).reshape(KV * 16, 128)
    hid = jnp.concatenate(
        [e2_f[pl.ds(c, KV, stride=16), :].astype(BF16) for c in range(11)], axis=1
    )
    down = jnp.dot(hid, wd[...], preferred_element_type=F32)
    f_s[...] = down.T.astype(BF16).reshape(TP, 16, KV)

    for k in (4, 5, 3, 2, 6, 7, 1):
        p = tp_peer(k)
        send(f_s.at[p], f_r.at[tp], f_ss, f_rs, (kv, p))
    f_r[tp] = f_s[tp]
    all_in(f_r.at[pl.ds(0, TP - 1)], f_rs)
    feed = jnp.sum(f_r[...].astype(F32), axis=0).astype(BF16).astype(F32)
    out_ref[...] = (mid_t[tp] + feed).astype(BF16)

    def all_out(ref, sem):
        pltpu.make_async_copy(ref, ref, sem).wait()

    all_out(tok.at[pl.ds(0, TP - 1)], tok_ss)
    all_out(b1_s.at[pl.ds(0, (KV - 1) * 8)], b1_ss)
    all_out(b2_r.at[pl.ds(0, KV - 1)], b2_ss)
    all_out(c1_s.at[pl.ds(0, KV - 1)], c1_ss)
    all_out(c2_r.at[pl.ds(0, KV - 1)], c2_ss)
    all_out(d_r.at[pl.ds(0, TP - 1)], d_ss)
    all_out(e1_s.at[pl.ds(0, (KV - 1) * 3)], e1_ss)
    all_out(e2_r.at[pl.ds(0, KV - 1)], e2_ss)
    all_out(f_s.at[pl.ds(0, TP - 1)], f_ss)


def shards(
    tokens, attention_norm_gain, query_first, query_second, key_first, key_second, value_weight,
    key_cache, value_cache, lambdas, head_gain, out_weight, mlp_gain, gate_weight, up_weight,
    down_projection_weight,
):
    hbm = pl.BlockSpec(memory_space=pl.ANY)
    vmem = pl.BlockSpec(memory_space=pltpu.VMEM)
    dma = pltpu.SemaphoreType.DMA
    out, kp, nv = pl.pallas_call(
        kernel,
        out_shape=(
            jax.ShapeDtypeStruct((16, KV), BF16),
            jax.ShapeDtypeStruct((KV, 128), BF16),
            jax.ShapeDtypeStruct((KV, 128), BF16),
        ),
        in_specs=[hbm] * 16,
        out_specs=(vmem, vmem, vmem),
        scratch_shapes=[
            pltpu.VMEM((1, 128), F32),
            pltpu.VMEM((128, 256), BF16),
            pltpu.VMEM((128, 256), BF16),
            pltpu.VMEM((128, 512), BF16),
            pltpu.VMEM((128, 128), BF16),
            pltpu.VMEM((128, 128), BF16),
            pltpu.VMEM((KV, 512, 128), BF16),
            pltpu.VMEM((KV, 512, 128), BF16),
            pltpu.SMEM((4,), F32),
            pltpu.VMEM((1, 128), F32),
            pltpu.VMEM((512, 128), BF16),
            pltpu.VMEM((1, 128), F32),
            pltpu.VMEM((128, 1408), BF16),
            pltpu.VMEM((128, 1408), BF16),
            pltpu.VMEM((1408, 128), BF16),
            pltpu.VMEM((TP, 16, KV), BF16),
            pltpu.VMEM((KV * 8, 128), F32),
            pltpu.VMEM((KV * 8, 128), F32),
            pltpu.VMEM((8, 128), BF16),
            pltpu.VMEM((KV, 8, 128), BF16),
            pltpu.VMEM((KV, 16, 128), BF16),
            pltpu.VMEM((KV, 16, 128), BF16),
            pltpu.VMEM((8, 128), BF16),
            pltpu.VMEM((KV, 8, 128), BF16),
            pltpu.VMEM((KV * 8, 128), F32),
            pltpu.VMEM((KV, 128), BF16),
            pltpu.VMEM((TP, KV, 128), BF16),
            pltpu.VMEM((KV * 24, 128), F32),
            pltpu.VMEM((KV * 3, 8, 128), BF16),
            pltpu.VMEM((KV * 3, 8, 128), BF16),
            pltpu.VMEM((16, 128), BF16),
            pltpu.VMEM((KV, 16, 128), BF16),
            pltpu.VMEM((KV * 16, 128), F32),
            pltpu.VMEM((TP, 16, KV), F32),
            pltpu.VMEM((TP, 16, KV), BF16),
            pltpu.VMEM((TP, 16, KV), BF16),
            dma((24,)),
            dma(()), dma(()), dma(()), dma(()), dma(()), dma((KV,)), dma(()), dma(()), dma(()),
            dma(()), dma(()), dma(()), dma(()), dma(()), dma(()), dma(()), dma(()), dma(()),
        ],
        compiler_params=pltpu.CompilerParams(collective_id=0, has_side_effects=True),
        name="decode_layer",
    )(
        tokens.T,
        attention_norm_gain.reshape(1, 128),
        query_first,
        query_second,
        key_first.T,
        key_second.T,
        value_weight,
        key_cache.reshape(KV, 512, 128),
        value_cache.reshape(KV, 512, 128),
        lambdas,
        head_gain.reshape(1, 128),
        out_weight,
        mlp_gain.reshape(1, 128),
        gate_weight,
        up_weight,
        down_projection_weight,
    )
    return out.T, kp[:, None, :], nv[:, None, :]


def solution(mesh):
    in_specs = (
        P(None, ("kv", "tp")),
        P("kv"),
        P("kv", "tp"),
        P("kv", "tp"),
        P("kv", "tp"),
        P("kv", "tp"),
        P("kv", "tp"),
        P(None, "kv", "tp", None),
        P(None, "kv", "tp", None),
        P("tp"),
        P(),
        P("tp", "kv"),
        P("kv"),
        P("kv", "tp"),
        P("kv", "tp"),
        P("tp", "kv"),
    )
    out_specs = (P(None, ("kv", "tp")), P(None, "tp", None), P(None, "tp", None))
    return jax.shard_map(shards, mesh=mesh, in_specs=in_specs, out_specs=out_specs, check_vma=False)
```

```python
import functools

import jax
import jax.numpy as jnp
from jax import lax
from jax.experimental import pallas as pl
from jax.experimental.pallas import tpu as pltpu
from jax.sharding import PartitionSpec as P

D = 4096
HD = 64
EPS = 1e-06
NZ, NY = 8, 4
KV = NZ * NY
TP = 8
F32 = jnp.float32
BF16 = jnp.bfloat16
MESH = pl.DeviceIdType.MESH

Z_DIST = [min(k, NZ - k) for k in range(NZ)]
Y_DIST = [min(k, NY - k) for k in range(NY)]
OFFSETS = sorted(
    [(dz, dy) for dz in range(NZ) for dy in range(NY) if (dz, dy) != (0, 0)],
    key=lambda o: -(Z_DIST[o[0]] + Y_DIST[o[1]]),
)


def kernel(
    tok_h, an_gain_h, wq1_h, wq2_h, wk1_h, wk2_h, wv_h, k_h, v_h, lam_h, hg_h, wo_h, mg_h, wg_h,
    wu_h, wd_h,
    out_ref, kp_ref, nv_ref,
    an_gain, wq1, wq2, wq, wk, wv, keys, vals, lam, hg, wo, mg, wg, wu, wd,
    tok, b1_s, b1_r, b2_s, b2_r, c1_s, c1_r, c2_s, c2_r, c2_f, d_s, d_r, e1_f, e1_s, e1_r, e2_s,
    e2_r, e2_f, mid_t, f_s, f_r, keys_t, s_scr,
    ld, tok_ss, tok_rs, b1_ss, b1_rs, b2_ss, b2_rs, c1_ss, c1_rs, c2_ss, c2_rs, d_ss, d_rs,
    e1_ss, e1_rs, e2_ss, e2_rs, f_ss, f_rs,
):
    kv = lax.axis_index("kv")
    tp = lax.axis_index("tp")
    mz, my = kv // NY, kv % NY

    def kv_peer(dz, dy):
        return ((mz + dz) % NZ) * NY + (my + dy) % NY

    def tp_peer(k):
        return (tp + k) % TP

    loads = []

    def load(src, dst):
        copy = pltpu.make_async_copy(src, dst, ld.at[len(loads)])
        copy.start()
        loads.append(copy)
        return copy

    l_tok = load(tok_h, tok.at[tp])
    l_ag = load(an_gain_h, an_gain)
    l_w = [
        load(wq1_h, wq1), load(wq2_h, wq2), load(wk1_h, wk.at[pl.ds(0, HD)]),
        load(wk2_h, wk.at[pl.ds(HD, HD)]), load(wv_h, wv),
    ]

    barrier = pltpu.get_barrier_semaphore()
    for dz, dy in OFFSETS:
        pl.semaphore_signal(barrier, inc=1, device_id=(kv_peer(dz, dy), tp), device_id_type=MESH)
    for k in range(1, TP):
        pl.semaphore_signal(barrier, inc=1, device_id=(kv, tp_peer(k)), device_id_type=MESH)

    l_k = [load(k_h.at[pl.ds(8 * i, 8)], keys.at[pl.ds(8 * i, 8)]) for i in range(4)]
    l_v = [load(v_h.at[pl.ds(8 * i, 8)], vals.at[pl.ds(8 * i, 8)]) for i in range(4)]
    l_lam = load(lam_h, lam)
    l_hg = load(hg_h, hg)
    l_wo = load(wo_h, wo)
    l_mg = load(mg_h, mg)
    l_gu = [load(wg_h, wg), load(wu_h, wu)]
    l_wd = load(wd_h, wd)

    def send(src, dst, ss, rs, device):
        copy = pltpu.make_async_remote_copy(
            src_ref=src, dst_ref=dst, send_sem=ss, recv_sem=rs, device_id=device,
            device_id_type=MESH,
        )
        copy.start()

    def all_in(ref, sem):
        pltpu.make_async_copy(ref, ref, sem).wait()

    for c in l_w:
        c.wait()
    for h in range(4):
        wq[:, 128 * h : 128 * h + 128] = jnp.concatenate(
            [wq1[:, HD * h : HD * h + HD], wq2[:, HD * h : HD * h + HD]], axis=1
        )
    b1_s[...] = jnp.zeros_like(b1_s)
    e1_f[...] = jnp.zeros_like(e1_f)
    l_tok.wait()
    l_ag.wait()
    pl.semaphore_wait(barrier, KV - 1 + TP - 1)

    for k in (4, 5, 3, 2, 6, 7, 1):
        send(tok.at[tp], tok.at[tp], tok_ss, tok_rs, (kv, tp_peer(k)))
    all_in(tok.at[pl.ds(0, TP - 1)], tok_rs)
    x = tok[...].astype(F32).reshape(TP * 16, KV).T
    scaled = (x * an_gain[...]).astype(BF16)
    sq = jnp.sum(x * x, axis=1, keepdims=True)
    b1_s[pl.ds(6, KV, stride=8), :] = jnp.broadcast_to(sq, (KV, 128))
    pq = jnp.dot(scaled, wq[...], preferred_element_type=F32)
    for h in range(4):
        b1_s[pl.ds(h, KV, stride=8), :] = pq[:, 128 * h : 128 * h + 128]
    b1_s[pl.ds(4, KV, stride=8), :] = lax.dot_general(
        scaled, wk[...], (((1,), (1,)), ((), ())), preferred_element_type=F32
    )
    b1_s[pl.ds(5, KV, stride=8), :] = jnp.dot(scaled, wv[...], preferred_element_type=F32)

    def rows(ref, i, n):
        return ref.at[pl.ds(pl.multiple_of(i * n, n), n)]

    for dz, dy in OFFSETS:
        p = kv_peer(dz, dy)
        send(rows(b1_s, p, 8), rows(b1_r, kv, 8), b1_ss, b1_rs, (p, tp))
    own = pl.ds(pl.multiple_of(kv * 8, 8), 8)
    b1_r[own, :] = b1_s[own, :]
    for c in l_k + l_v:
        c.wait()

    def turn(s, carry):
        keys_t[s] = keys[s].T
        return carry

    lax.fori_loop(0, KV, turn, 0, unroll=2)
    all_in(b1_r.at[pl.ds(0, (KV - 1) * 8)], b1_rs)
    total = jnp.sum(b1_r[...].reshape(KV, 8, 128), axis=0)
    factor = lax.rsqrt(total[6:7] / D + EPS)
    proj = (total * factor).astype(BF16).astype(F32)
    lane = lax.broadcasted_iota(jnp.int32, (8, 128), 1)
    row = lax.broadcasted_iota(jnp.int32, (8, 128), 0)
    both = jnp.concatenate([proj[0:4], proj[0:4]], axis=0)
    query = jnp.where((lane < HD) == (row < 4), both, 0.0) * HD ** (-0.5)
    b2_s[...] = query.astype(BF16)

    for dz, dy in OFFSETS:
        send(b2_s, b2_r.at[kv], b2_ss, b2_rs.at[kv], (kv_peer(dz, dy), tp))
    b2_r[kv] = query.astype(BF16)
    new_key, new_value = proj[4:5], proj[5:6]
    fresh = jnp.sum(query * new_key, axis=1, keepdims=True)

    def plane(g):
        half = (g + 1) // 2
        dz = (g % 2) * half + (1 - g % 2) * ((NZ - half) % NZ)
        return ((mz + dz) % NZ) * NY

    def arrive(g):
        for j in range(NY):
            s = plane(g) + j

            @pl.when(s != kv)
            def _():
                pltpu.make_async_copy(b2_r.at[s], b2_r.at[s], b2_rs.at[s]).wait()

    def scores(g):
        return [
            jnp.dot(b2_r[plane(g) + j], keys_t[plane(g) + j], preferred_element_type=F32)
            for j in range(NY)
        ]

    def values(g, score):
        top = [jnp.max(t, axis=1, keepdims=True) for t in score]
        expo = [jnp.exp(t - m) for t, m in zip(score, top)]
        acc = [
            jnp.dot(e.astype(BF16), vals[plane(g) + j], preferred_element_type=F32)
            for j, e in enumerate(expo)
        ]
        for j in range(NY):
            tot = jnp.sum(expo[j], axis=1, keepdims=True)
            level = jnp.broadcast_to(top[j] + jnp.log(tot), (8, 128))
            p1 = level.astype(BF16).astype(F32)
            p2 = (level - p1).astype(BF16).astype(F32)
            p3 = level - p1 - p2
            pieces = jnp.where(
                lane == 0, p1, jnp.where(lane == 1, p2, jnp.where(lane == 2, p3, 0.0))
            )
            c1_s[plane(g) + j] = jnp.concatenate([acc[j] / tot, pieces], axis=0).astype(BF16)

    def depart(g):
        for j in range(NY):
            s = plane(g) + j

            @pl.when(s != kv)
            def _():
                send(c1_s.at[s], c1_r.at[kv], c1_ss, c1_rs, (s, tp))

    def attend(g, carry):
        arrive(g)
        before = [s_scr[(g + 1) % 2, j] for j in range(NY)]
        now = scores(g)
        values(g - 1, before)
        for j in range(NY):
            s_scr[g % 2, j] = now[j]
        depart(g - 1)
        return carry

    arrive(0)
    for j, t in enumerate(scores(0)):
        s_scr[0, j] = t
    lax.fori_loop(1, NZ, attend, 0)
    values(NZ - 1, [s_scr[(NZ - 1) % 2, j] for j in range(NY)])
    depart(NZ - 1)
    c1_r[kv] = c1_s[kv]

    for c in (l_lam, l_hg, l_wo, l_mg):
        c.wait()
    r4 = lax.broadcasted_iota(jnp.int32, (4, 128), 0)
    lam_rows = jnp.where(
        r4 == 0, lam[0], jnp.where(r4 == 1, lam[1], jnp.where(r4 == 2, lam[2], lam[3]))
    )
    all_in(c1_r.at[pl.ds(0, KV - 1)], c1_rs)
    states = c1_r[...].astype(F32)
    values = states[:, 0:8, :]
    levels = jnp.sum(states[:, 8:16, :], axis=2, keepdims=True)
    top = jnp.maximum(jnp.max(levels, axis=0), fresh)
    weight = jnp.exp(levels - top[None])
    fresh_weight = jnp.exp(fresh - top)
    total_w = jnp.sum(weight, axis=0) + fresh_weight
    merged = (jnp.sum(values * weight, axis=0) + fresh_weight * new_value) / total_w
    mixed = merged[0:4] - lam_rows * merged[4:8]
    normed = (
        mixed * lax.rsqrt(jnp.mean(mixed * mixed, axis=1, keepdims=True) + EPS) * hg[...]
    )
    c2 = jnp.concatenate([normed, proj[4:6], jnp.zeros((2, 128), F32)], axis=0).astype(BF16)
    c2_s[...] = c2

    for dz, dy in OFFSETS:
        send(c2_s, c2_r.at[kv], c2_ss, c2_rs, (kv_peer(dz, dy), tp))
    c2_r[kv] = c2
    all_in(c2_r.at[pl.ds(0, KV - 1)], c2_rs)
    c2_f[...] = c2_r[...].astype(F32).reshape(KV * 8, 128)
    heads = jnp.concatenate(
        [c2_f[pl.ds(h, KV, stride=8), :].astype(BF16) for h in range(4)], axis=1
    )
    attn_part = jnp.dot(heads, wo[...], preferred_element_type=F32).astype(BF16)
    d_s[...] = attn_part

    for k in (4, 5, 3, 2, 6, 7, 1):
        send(d_s, d_r.at[tp], d_ss, d_rs, (kv, tp_peer(k)))
    d_r[tp] = attn_part
    kp_ref[...] = c2_f[pl.ds(4, KV, stride=8), :].astype(BF16)
    nv_ref[...] = c2_f[pl.ds(5, KV, stride=8), :].astype(BF16)
    all_in(d_r.at[pl.ds(0, TP - 1)], d_rs)
    attn = jnp.sum(d_r[...].astype(F32), axis=0).astype(BF16).astype(F32)
    middle = (x + attn).astype(BF16).astype(F32)
    scaled_mid = (middle * mg[...]).astype(BF16)
    sq_mid = jnp.broadcast_to(jnp.sum(middle * middle, axis=1, keepdims=True), (KV, 128))
    for c in l_gu:
        c.wait()
    lane32 = lax.broadcasted_iota(jnp.int32, (KV, 128), 1)
    s1 = sq_mid.astype(BF16).astype(F32)
    s2 = (sq_mid - s1).astype(BF16).astype(F32)
    e1_f[pl.ds(22, KV, stride=24), :] = jnp.where(
        lane32 == 0, s1, jnp.where(lane32 == 1, s2, jnp.where(lane32 == 2, sq_mid - s1 - s2, 0.0))
    )
    gate = jnp.dot(scaled_mid, wg[...], preferred_element_type=F32)
    for c in range(11):
        e1_f[pl.ds(c, KV, stride=24), :] = gate[:, 128 * c : 128 * c + 128]
    up = jnp.dot(scaled_mid, wu[...], preferred_element_type=F32)
    for c in range(11):
        e1_f[pl.ds(11 + c, KV, stride=24), :] = up[:, 128 * c : 128 * c + 128]
    e1_s[...] = e1_f[...].reshape(KV * 3, 8, 128).astype(BF16)

    def thirds(ref, i):
        return ref.at[pl.ds(i * 3, 3)]

    for dz, dy in OFFSETS:
        p = kv_peer(dz, dy)
        send(thirds(e1_s, p), thirds(e1_r, kv), e1_ss, e1_rs, (p, tp))
    e1_r[pl.ds(kv * 3, 3)] = e1_s[pl.ds(kv * 3, 3)]
    mid_t[...] = middle.T.reshape(TP, 16, KV)
    all_in(e1_r.at[pl.ds(0, (KV - 1) * 3)], e1_rs)
    sums = jnp.sum(e1_r[...].astype(F32).reshape(KV, 24, 128), axis=0)
    factor_mid = lax.rsqrt(jnp.sum(sums[22:23], axis=1, keepdims=True) / D + EPS)
    gate_all = sums[0:11] * factor_mid
    up_all = sums[11:22] * factor_mid
    hidden = gate_all / (1.0 + jnp.exp(-gate_all)) * up_all
    hidden = jnp.concatenate([hidden, jnp.zeros((5, 128), F32)], axis=0).astype(BF16)
    e2_s[...] = hidden

    for dz, dy in OFFSETS:
        send(e2_s, e2_r.at[kv], e2_ss, e2_rs, (kv_peer(dz, dy), tp))
    e2_r[kv] = hidden
    l_wd.wait()
    all_in(e2_r.at[pl.ds(0, KV - 1)], e2_rs)
    e2_f[...] = e2_r[...].astype(F32).reshape(KV * 16, 128)
    hid = jnp.concatenate(
        [e2_f[pl.ds(c, KV, stride=16), :].astype(BF16) for c in range(11)], axis=1
    )
    down = jnp.dot(hid, wd[...], preferred_element_type=F32)
    f_s[...] = down.T.astype(BF16).reshape(TP, 16, KV)

    for k in (4, 5, 3, 2, 6, 7, 1):
        p = tp_peer(k)
        send(f_s.at[p], f_r.at[tp], f_ss, f_rs, (kv, p))
    f_r[tp] = f_s[tp]
    all_in(f_r.at[pl.ds(0, TP - 1)], f_rs)
    feed = jnp.sum(f_r[...].astype(F32), axis=0).astype(BF16).astype(F32)
    out_ref[...] = (mid_t[tp] + feed).astype(BF16)

    def all_out(ref, sem):
        pltpu.make_async_copy(ref, ref, sem).wait()

    all_out(tok.at[pl.ds(0, TP - 1)], tok_ss)
    all_out(b1_s.at[pl.ds(0, (KV - 1) * 8)], b1_ss)
    all_out(b2_r.at[pl.ds(0, KV - 1)], b2_ss)
    all_out(c1_s.at[pl.ds(0, KV - 1)], c1_ss)
    all_out(c2_r.at[pl.ds(0, KV - 1)], c2_ss)
    all_out(d_r.at[pl.ds(0, TP - 1)], d_ss)
    all_out(e1_s.at[pl.ds(0, (KV - 1) * 3)], e1_ss)
    all_out(e2_r.at[pl.ds(0, KV - 1)], e2_ss)
    all_out(f_s.at[pl.ds(0, TP - 1)], f_ss)


def hand_over(a_ref, b_ref, c_ref, x_ref, y_ref, z_ref):
    x_ref[...] = a_ref[...]
    y_ref[...] = b_ref[...]
    z_ref[...] = c_ref[...]


def shards(
    tokens, attention_norm_gain, query_first, query_second, key_first, key_second, value_weight,
    key_cache, value_cache, lambdas, head_gain, out_weight, mlp_gain, gate_weight, up_weight,
    down_projection_weight,
):
    hbm = pl.BlockSpec(memory_space=pltpu.HBM)
    vmem = pl.BlockSpec(memory_space=pltpu.VMEM)
    dma = pltpu.SemaphoreType.DMA
    out, kp, nv = pl.pallas_call(
        kernel,
        out_shape=(
            pltpu.VMEM((16, KV), BF16),
            pltpu.VMEM((KV, 128), BF16),
            pltpu.VMEM((KV, 128), BF16),
        ),
        in_specs=[hbm] * 16,
        out_specs=(vmem, vmem, vmem),
        scratch_shapes=[
            pltpu.VMEM((1, 128), F32),
            pltpu.VMEM((128, 256), BF16),
            pltpu.VMEM((128, 256), BF16),
            pltpu.VMEM((128, 512), BF16),
            pltpu.VMEM((128, 128), BF16),
            pltpu.VMEM((128, 128), BF16),
            pltpu.VMEM((KV, 512, 128), BF16),
            pltpu.VMEM((KV, 512, 128), BF16),
            pltpu.SMEM((4,), F32),
            pltpu.VMEM((1, 128), F32),
            pltpu.VMEM((512, 128), BF16),
            pltpu.VMEM((1, 128), F32),
            pltpu.VMEM((128, 1408), BF16),
            pltpu.VMEM((128, 1408), BF16),
            pltpu.VMEM((1408, 128), BF16),
            pltpu.VMEM((TP, 16, KV), BF16),
            pltpu.VMEM((KV * 8, 128), F32),
            pltpu.VMEM((KV * 8, 128), F32),
            pltpu.VMEM((8, 128), BF16),
            pltpu.VMEM((KV, 8, 128), BF16),
            pltpu.VMEM((KV, 16, 128), BF16),
            pltpu.VMEM((KV, 16, 128), BF16),
            pltpu.VMEM((8, 128), BF16),
            pltpu.VMEM((KV, 8, 128), BF16),
            pltpu.VMEM((KV * 8, 128), F32),
            pltpu.VMEM((KV, 128), BF16),
            pltpu.VMEM((TP, KV, 128), BF16),
            pltpu.VMEM((KV * 24, 128), F32),
            pltpu.VMEM((KV * 3, 8, 128), BF16),
            pltpu.VMEM((KV * 3, 8, 128), BF16),
            pltpu.VMEM((16, 128), BF16),
            pltpu.VMEM((KV, 16, 128), BF16),
            pltpu.VMEM((KV * 16, 128), F32),
            pltpu.VMEM((TP, 16, KV), F32),
            pltpu.VMEM((TP, 16, KV), BF16),
            pltpu.VMEM((TP, 16, KV), BF16),
            pltpu.VMEM((KV, 128, 512), BF16),
            pltpu.VMEM((2, NY, 8, 512), F32),
            dma((24,)),
            dma(()), dma(()), dma(()), dma(()), dma(()), dma((KV,)), dma(()), dma(()), dma(()),
            dma(()), dma(()), dma(()), dma(()), dma(()), dma(()), dma(()), dma(()), dma(()),
        ],
        compiler_params=pltpu.CompilerParams(
            collective_id=0, has_side_effects=True
        ),
        name="decode_layer",
    )(
        tokens.T,
        attention_norm_gain.reshape(1, 128),
        query_first,
        query_second,
        key_first.T,
        key_second.T,
        value_weight,
        key_cache.reshape(KV, 512, 128),
        value_cache.reshape(KV, 512, 128),
        lambdas,
        head_gain.reshape(1, 128),
        out_weight,
        mlp_gain.reshape(1, 128),
        gate_weight,
        up_weight,
        down_projection_weight,
    )
    out, kp, nv = pl.pallas_call(
        hand_over,
        out_shape=(
            jax.ShapeDtypeStruct((16, KV), BF16),
            jax.ShapeDtypeStruct((KV, 128), BF16),
            jax.ShapeDtypeStruct((KV, 128), BF16),
        ),
        in_specs=[vmem] * 3,
        out_specs=(vmem, vmem, vmem),
        compiler_params=pltpu.CompilerParams(vmem_limit_bytes=2**20),
        name="hand_over",
    )(out, kp, nv)
    return out.T, kp[:, None, :], nv[:, None, :]


def solution(mesh):
    in_specs = (
        P(None, ("kv", "tp")),
        P("kv"),
        P("kv", "tp"),
        P("kv", "tp"),
        P("kv", "tp"),
        P("kv", "tp"),
        P("kv", "tp"),
        P(None, "kv", "tp", None),
        P(None, "kv", "tp", None),
        P("tp"),
        P(),
        P("tp", "kv"),
        P("kv"),
        P("kv", "tp"),
        P("kv", "tp"),
        P("tp", "kv"),
    )
    out_specs = (P(None, ("kv", "tp")), P(None, "tp", None), P(None, "tp", None))
    return jax.shard_map(shards, mesh=mesh, in_specs=in_specs, out_specs=out_specs, check_vma=False)
```
